32 devices in a mesh: fs: 8 (over z, x), tp: 4 (over y, core).
Axes of the slice: x: 2, y: 2, z: 4, core: 2. Of those that a mesh axis runs over, the one named last changes fastest.
Arguments:
- block_input: bfloat16 [8192, 2048], P(('fs', 'tp')), may hold values from -6 to 6
- gate_cotangent: bfloat16 [8192, 2048], P('fs', 'tp'), may hold values from -0.06591797 to 0.06591797
- gated_state: bfloat16 [8192, 2048], P('fs', 'tp'), may hold values from -6 to 6
- mixer_cotangent: bfloat16 [8192, 2048], P(('fs', 'tp')), may hold values from -0.06591797 to 0.06591797
- gate_basis: bfloat16 [2048, 512], P('fs'), may hold values from -0.125 to 0.125
- out_basis: bfloat16 [2048, 512], P('fs'), may hold values from -0.125 to 0.125
- gate_master: float32 [2048, 2048], P('fs', 'tp'), may hold values from -0.6 to 0.6
- out_master: float32 [2048, 2048], P('tp', 'fs'), may hold values from -0.6 to 0.6
- gate_first: float32 [512, 2048], P('fs', 'tp'), may hold values from -3 to 3
- gate_second: float32 [512, 2048], P('fs', 'tp'), may hold values from 0.01 to 8.1, as said below
- out_first: float32 [512, 2048], P('fs', 'tp'), may hold values from -3 to 3
- out_second: float32 [512, 2048], P('fs', 'tp'), may hold values from 0.01 to 8.1, as said below
Outputs:
- gate_master_new: float32 [2048, 2048], P('fs', 'tp')
- out_master_new: float32 [2048, 2048], P('tp', 'fs')
- gate_copy: bfloat16 [2048, 2048], P(None, 'tp')
- out_copy: bfloat16 [2048, 2048], P('tp')
- gate_first_new: float32 [512, 2048], P('fs', 'tp')
- gate_second_new: float32 [512, 2048], P('fs', 'tp')
- out_first_new: float32 [512, 2048], P('fs', 'tp')
- out_second_new: float32 [512, 2048], P('fs', 'tp')
The draws below stay inside these ranges and needn't reach their ends.
Inputs may be any that keep to these rules, and one draw needn't show every extreme that they name: `gate_second`: positive. `out_second`: positive.
All inputs are finite; a program needn't handle non-finite values.
Results may differ from the reference program's by a relative error of at most 0.0038.
Values may be sent and summed in bfloat16 or wider, within the bound.
No kernel may reach another device: no remote copies, remote signals or barrier semaphores. Data moves between devices by JAX's collectives and lax.ppermute only.
A program may use at most 64 MiB of HBM per device.

```python
import math
import jax
import jax.numpy as jnp
from jax import lax

D = 2048
DI = 2048
R = 512
TOKENS = 8192


def second_moment(key):
    row_frac = jnp.arange(R, dtype=jnp.float32)[:, None] / R
    col_frac = jnp.arange(DI, dtype=jnp.float32)[None, :] / DI
    jitter = jax.random.uniform(key, (R, DI), jnp.float32, 0.0, 1.0)
    slope = row_frac + col_frac
    return 0.01 * jnp.exp(jitter * math.log(10.0) + slope * math.log(9.0))


def draw_gate_second(key, part):
    return second_moment(jax.random.fold_in(key, 11))


def draw_out_second(key, part):
    return second_moment(jax.random.fold_in(key, 12))


def levels(stream_key, extent, shards, low, top_value):
    loudness, own = 1.0, jax.random.fold_in(stream_key, 6)
    for axis_at, parts in shards:
        draws = jnp.exp(jax.random.uniform(jax.random.fold_in(own, axis_at), (parts,), jnp.float32, low / len(shards), top_value / len(shards)))
        loudness = loudness * jnp.repeat(draws, extent[axis_at] // parts).reshape([-1 if axis == axis_at else 1 for axis in range(len(extent))])
    return loudness


def gaussian(stream_key, shape, width, bound, split=(), kind=jnp.bfloat16):
    loudness = levels(stream_key, shape, split, -0.22, 0.18) if split else 1.0
    entries = jax.random.normal(stream_key, shape, jnp.float32) * width * loudness
    return jnp.minimum(jnp.maximum(entries, -bound), bound).astype(kind)


def setup_inputs(seed: int = 0) -> dict:
    splits = jax.random.split(jax.random.key(seed), 13)
    return {
        "block_input": gaussian(splits[0], (TOKENS, D), 1.0, 6.0, ((0, 32),)),
        "gate_cotangent": gaussian(splits[1], (TOKENS, DI), (TOKENS ** -0.5), 0.06591797, ((0, 8), (1, 4))),
        "gated_state": gaussian(splits[2], (TOKENS, DI), 1.0, 6.0, ((0, 8), (1, 4))),
        "mixer_cotangent": gaussian(splits[3], (TOKENS, D), (TOKENS ** -0.5), 0.06591797, ((0, 32),)),
        "gate_basis": gaussian(splits[4], (D, R), D ** -0.5, 0.125, ((0, 8),)),
        "out_basis": gaussian(splits[5], (D, R), D ** -0.5, 0.125, ((0, 8),)),
        "gate_master": gaussian(splits[6], (D, DI), 0.1, 0.6, ((0, 8), (1, 4)), jnp.float32),
        "out_master": gaussian(splits[7], (DI, D), 0.1, 0.6, ((0, 4), (1, 8)), jnp.float32),
        "gate_first": gaussian(splits[8], (R, DI), 0.5, 3.0, ((0, 8), (1, 4)), jnp.float32),
        "gate_second": draw_gate_second(jax.random.fold_in(splits[12], 71), 0),
        "out_first": gaussian(splits[10], (R, DI), 0.5, 3.0, ((0, 8), (1, 4)), jnp.float32),
        "out_second": draw_out_second(jax.random.fold_in(splits[12], 71), 0),
    }


def reference(block_input, gate_cotangent, gated_state, mixer_cotangent, gate_basis, out_basis, gate_master, out_master, gate_first, gate_second, out_first, out_second):
    proj_in = jnp.dot(block_input, gate_basis, preferred_element_type=jnp.float32).astype(jnp.bfloat16)
    proj_cot = jnp.dot(mixer_cotangent, out_basis, preferred_element_type=jnp.float32).astype(jnp.bfloat16)
    contract = (((0,), (0,)), ((), ()))
    gate_low = lax.dot_general(proj_in, gate_cotangent, contract, preferred_element_type=jnp.float32)
    out_low = lax.dot_general(proj_cot, gated_state, contract, preferred_element_type=jnp.float32)
    gate_first_new = 0.9 * gate_first + 0.1 * gate_low
    out_first_new = 0.9 * out_first + 0.1 * out_low
    gate_second_new = 0.95 * gate_second + 0.05 * gate_low * gate_low
    out_second_new = 0.95 * out_second + 0.05 * out_low * out_low
    gate_raw = gate_first_new / jnp.sqrt(gate_second_new)
    out_raw = out_first_new / jnp.sqrt(out_second_new)
    squares = jnp.sum(gate_raw * gate_raw) + jnp.sum(out_raw * out_raw)
    norm_scale = lax.rsqrt(squares / (2.0 * R * DI) + 1e-06)
    gate_update = jnp.dot(gate_basis.astype(jnp.float32), gate_raw * norm_scale, precision=lax.Precision.HIGHEST)
    out_update = lax.dot_general(out_raw * norm_scale, out_basis.astype(jnp.float32), (((0,), (1,)), ((), ())), precision=lax.Precision.HIGHEST)
    gate_master_new = gate_master - 0.25 * gate_update
    out_master_new = out_master - 0.25 * out_update
    return (gate_master_new, out_master_new, gate_master_new.astype(jnp.bfloat16), out_master_new.astype(jnp.bfloat16), gate_first_new, gate_second_new, out_first_new, out_second_new)
```

```python
import jax
import jax.numpy as jnp
from jax import lax
from jax.sharding import PartitionSpec as P


UNROLL_LIMIT = 16


def ring_order(count):
    return list(range(0, count, 2)) + list(range(1, count, 2))[::-1]


def ring_chunks(own, axis, count):
    order = ring_order(count)
    place_of = [order.index(i) for i in range(count)]
    forward = [(order[p], order[(p + 1) % count]) for p in range(count)]
    backward = [(b, a) for a, b in forward]
    place = jnp.asarray(place_of, jnp.int32)[lax.axis_index(axis)]
    owner_at = jnp.asarray(order, jnp.int32)
    half = own.shape[0] // 2
    up = down = own
    chunks = []
    for step in range(1, count // 2):
        up = lax.ppermute(up, axis, forward)
        down = lax.ppermute(down, axis, backward)
        chunks.append((owner_at[(place - step) % count], 0, up))
        chunks.append((owner_at[(place + step) % count], 0, down))
    far = owner_at[(place + count // 2) % count]
    chunks.append((far, 0, lax.ppermute(up[:half], axis, forward)))
    chunks.append((far, half, lax.ppermute(down[half:], axis, backward)))
    return chunks


def gather_rows(own, axis, count):
    if count % 2 or count > UNROLL_LIMIT:
        return lax.all_gather(own, axis, axis=0, tiled=True)
    rows = own.shape[0]
    whole = jnp.zeros((count * rows, own.shape[1]), own.dtype)
    whole = lax.dynamic_update_slice_in_dim(whole, own, lax.axis_index(axis) * rows, 0)
    for owner, start, chunk in ring_chunks(own, axis, count):
        whole = lax.dynamic_update_slice_in_dim(whole, chunk, owner * rows + start, 0)
    return whole


def gather_bases(gate_basis, out_basis, fs_count, tp_count):
    if fs_count % 2 or tp_count % 2 or fs_count > UNROLL_LIMIT:
        return (
            lax.all_gather(gate_basis, "fs", axis=0, tiled=True),
            lax.all_gather(out_basis, "fs", axis=0, tiled=True),
        )
    rows, cols = gate_basis.shape
    parity = lax.axis_index("tp") % 2
    swap = [(i, i ^ 1) for i in range(tp_count)]
    own = jnp.where(parity == 0, gate_basis, out_basis)
    wholes = jnp.zeros((2, fs_count * rows, cols), gate_basis.dtype)
    at = lax.axis_index("fs") * rows
    wholes = lax.dynamic_update_slice(wholes, jnp.stack([gate_basis, out_basis]), (0, at, 0))
    for owner, start, chunk in ring_chunks(own, "fs", fs_count):
        other = lax.ppermute(chunk, "tp", swap)
        at = owner * rows + start
        wholes = lax.dynamic_update_slice(wholes, chunk[None], (parity, at, 0))
        wholes = lax.dynamic_update_slice(wholes, other[None], (1 - parity, at, 0))
    return wholes[0], wholes[1]


def butterfly(own, count):
    stack, stride = own, count // 2
    while stride:
        pairs = [(i, i ^ stride) for i in range(count)]
        stack = jnp.concatenate([stack, lax.ppermute(stack, "tp", pairs)], axis=0)
        stride //= 2
    return stack


def butterfly_order(count):
    order, stride = [0], count // 2
    while stride:
        order = order + [k ^ stride for k in order]
        stride //= 2
    return order


def sum_scatter(terms, axis, count):
    rows = terms.shape[0] // count
    me = lax.axis_index(axis)
    if count > UNROLL_LIMIT:
        return lax.psum_scatter(terms, axis, scatter_dimension=0, tiled=True)
    total = lax.dynamic_slice_in_dim(terms, me * rows, rows, 0)
    sent = terms.astype(jnp.bfloat16)
    for shift in range(1, count):
        piece = lax.dynamic_slice_in_dim(sent, ((me + shift) % count) * rows, rows, 0)
        pairs = [(i, (i + shift) % count) for i in range(count)]
        total = total + lax.ppermute(piece, axis, pairs).astype(jnp.float32)
    return total


def on_device(
    block_input,
    gate_cotangent,
    gated_state,
    mixer_cotangent,
    gate_basis,
    out_basis,
    gate_master,
    out_master,
    gate_first,
    gate_second,
    out_first,
    out_second,
):
    low_rank = gate_basis.shape[1]
    local_cols = gate_first.shape[1]
    fs_count, tp_count = lax.axis_size("fs"), lax.axis_size("tp")
    own_tokens = block_input.shape[0]
    member = lax.axis_index("tp")

    gate_old = lax.all_gather(gate_master.astype(jnp.bfloat16), "fs", axis=0, tiled=True)
    out_old = lax.all_gather(out_master.astype(jnp.bfloat16), "fs", axis=1, tiled=True)

    gate_whole, out_whole = gather_bases(gate_basis, out_basis, fs_count, tp_count)
    own_in = jnp.dot(block_input, gate_whole, preferred_element_type=jnp.float32)
    own_cot = jnp.dot(mixer_cotangent, out_whole, preferred_element_type=jnp.float32)
    own_in, own_cot = own_in.astype(jnp.bfloat16), own_cot.astype(jnp.bfloat16)

    if tp_count & (tp_count - 1):
        proj_in = lax.all_gather(own_in, "tp", axis=0, tiled=True)
        proj_cot = lax.all_gather(own_cot, "tp", axis=0, tiled=True)
        gate_right, out_right = gate_cotangent, gated_state
    else:
        proj_in, proj_cot = butterfly(own_in, tp_count), butterfly(own_cot, tp_count)
        blocks = [(member ^ k) * own_tokens for k in butterfly_order(tp_count)]
        gate_right, out_right = (
            jnp.concatenate([lax.dynamic_slice_in_dim(a, b, own_tokens, 0) for b in blocks])
            for a in (gate_cotangent, gated_state)
        )
    contract = (((0,), (0,)), ((), ()))
    gate_term = lax.dot_general(proj_in, gate_right, contract, preferred_element_type=jnp.float32)
    out_term = lax.dot_general(proj_cot, out_right, contract, preferred_element_type=jnp.float32)
    gate_low = sum_scatter(gate_term, "fs", fs_count)
    out_low = sum_scatter(out_term, "fs", fs_count)

    gate_first_new = 0.9 * gate_first + 0.1 * gate_low
    out_first_new = 0.9 * out_first + 0.1 * out_low
    gate_second_new = 0.95 * gate_second + 0.05 * gate_low * gate_low
    out_second_new = 0.95 * out_second + 0.05 * out_low * out_low
    raw_gate = gate_first_new / jnp.sqrt(gate_second_new)
    raw_out = out_first_new / jnp.sqrt(out_second_new)

    raw_step = jnp.concatenate([raw_gate, raw_out], axis=1).astype(jnp.bfloat16)
    full_step = gather_rows(raw_step, "fs", fs_count)
    wide_step = full_step.astype(jnp.float32)
    squares = jnp.full((8, 128), jnp.sum(wide_step * wide_step))
    parts = [squares]
    for shift in range(1, tp_count):
        pairs = [(i, (i + shift) % tp_count) for i in range(tp_count)]
        parts.append(lax.ppermute(squares, "tp", pairs))
    squares = sum(parts)[0, 0]
    norm_scale = lax.rsqrt(squares / (2.0 * low_rank * local_cols * tp_count) + 1e-06)
    rate = 0.25 * norm_scale

    full_gate, full_out = full_step[:, :local_cols], full_step[:, local_cols:]
    across = (((0,), (1,)), ((), ()))
    gate_copy = gate_old.astype(jnp.float32) - rate * jnp.dot(
        gate_whole, full_gate, preferred_element_type=jnp.float32
    )
    out_copy = out_old.astype(jnp.float32) - rate * lax.dot_general(
        full_out, out_whole, across, preferred_element_type=jnp.float32
    )
    gate_master_new = gate_master - rate * jnp.dot(
        gate_basis, full_gate, preferred_element_type=jnp.float32
    )
    out_master_new = out_master - rate * lax.dot_general(
        full_out, out_basis, across, preferred_element_type=jnp.float32
    )
    return (
        gate_master_new,
        out_master_new,
        gate_copy.astype(jnp.bfloat16),
        out_copy.astype(jnp.bfloat16),
        gate_first_new,
        gate_second_new,
        out_first_new,
        out_second_new,
    )


def solution(mesh):
    return jax.shard_map(
        on_device,
        mesh=mesh,
        in_specs=(
            P(("fs", "tp"), None),
            P("fs", "tp"),
            P("fs", "tp"),
            P(("fs", "tp"), None),
            P("fs", None),
            P("fs", None),
            P("fs", "tp"),
            P("tp", "fs"),
            P("fs", "tp"),
            P("fs", "tp"),
            P("fs", "tp"),
            P("fs", "tp"),
        ),
        out_specs=(
            P("fs", "tp"),
            P("tp", "fs"),
            P(None, "tp"),
            P("tp", None),
            P("fs", "tp"),
            P("fs", "tp"),
            P("fs", "tp"),
            P("fs", "tp"),
        ),
        check_vma=False,
    )
```

```python
import jax
import jax.numpy as jnp
from jax import lax
from jax.sharding import PartitionSpec as P


UNROLL_LIMIT = 16


def ring_order(count):
    return list(range(0, count, 2)) + list(range(1, count, 2))[::-1]


def ring_chunks(own, axis, count):
    order = ring_order(count)
    place_of = [order.index(i) for i in range(count)]
    forward = [(order[p], order[(p + 1) % count]) for p in range(count)]
    backward = [(b, a) for a, b in forward]
    place = jnp.asarray(place_of, jnp.int32)[lax.axis_index(axis)]
    owner_at = jnp.asarray(order, jnp.int32)
    half = own.shape[0] // 2
    up = down = own
    chunks = []
    for step in range(1, count // 2):
        up = lax.ppermute(up, axis, forward)
        down = lax.ppermute(down, axis, backward)
        chunks.append((owner_at[(place - step) % count], 0, up))
        chunks.append((owner_at[(place + step) % count], 0, down))
    far = owner_at[(place + count // 2) % count]
    chunks.append((far, 0, lax.ppermute(up[:half], axis, forward)))
    chunks.append((far, half, lax.ppermute(down[half:], axis, backward)))
    return chunks


def gather_steps(own, count):
    if count % 2 or count > UNROLL_LIMIT:
        return lax.all_gather(own, "fs", axis=1, tiled=True)
    me = lax.axis_index("fs")
    kinds, rows, cols = own.shape
    swap = [(i, i ^ 1) for i in range(count)]
    whole = jnp.zeros((kinds, count * rows, cols), own.dtype)
    for shift in sorted(range(0, count, 2), key=lambda k: -min(k, count - k) if k else 0):
        pairs = [(i, (i + shift) % count) for i in range(count)]
        piece = lax.ppermute(own, "fs", pairs) if shift else own
        owner = (me - shift) % count
        other = lax.ppermute(piece, "fs", swap)
        whole = lax.dynamic_update_slice(whole, piece, (0, owner * rows, 0))
        across = ((me ^ 1) - shift) % count
        whole = lax.dynamic_update_slice(whole, other, (0, across * rows, 0))
    return whole


def project(gate_input, out_input, gate_basis, out_basis, fs_count, tp_count):
    if fs_count % 2 or tp_count % 2 or fs_count > UNROLL_LIMIT:
        wholes = [
            lax.all_gather(basis, "fs", axis=0, tiled=True) for basis in (gate_basis, out_basis)
        ]
        terms = [
            jnp.dot(a, whole, preferred_element_type=jnp.float32)
            for a, whole in zip((gate_input, out_input), wholes)
        ]
        return terms[0], terms[1], wholes[0], wholes[1]
    rows, cols = gate_basis.shape
    even = lax.axis_index("tp") % 2 == 0
    parity = lax.axis_index("tp") % 2
    swap = [(i, i ^ 1) for i in range(tp_count)]
    own = jnp.where(even, gate_basis, out_basis)
    other = jnp.where(even, out_basis, gate_basis)
    own_input = jnp.where(even, gate_input, out_input)
    other_input = jnp.where(even, out_input, gate_input)

    def part(whole_input, at, chunk):
        cut = lax.dynamic_slice_in_dim(whole_input, at, chunk.shape[0], 1)
        return jnp.dot(cut, chunk, preferred_element_type=jnp.float32)

    at = lax.axis_index("fs") * rows
    own_sum, other_sum = part(own_input, at, own), part(other_input, at, other)
    wholes = jnp.zeros((2, fs_count * rows, cols), gate_basis.dtype)
    wholes = lax.dynamic_update_slice(wholes, jnp.stack([gate_basis, out_basis]), (0, at, 0))
    for owner, start, chunk in ring_chunks(own, "fs", fs_count):
        other = lax.ppermute(chunk, "tp", swap)
        at = owner * rows + start
        own_sum = own_sum + part(own_input, at, chunk)
        other_sum = other_sum + part(other_input, at, other)
        wholes = lax.dynamic_update_slice(wholes, chunk[None], (parity, at, 0))
        wholes = lax.dynamic_update_slice(wholes, other[None], (1 - parity, at, 0))
    gate_sum = jnp.where(even, own_sum, other_sum)
    out_sum = jnp.where(even, other_sum, own_sum)
    return gate_sum, out_sum, wholes[0], wholes[1]


def token_blocks(own, count):
    blocks, stride = [(0, own)], count // 2
    while stride:
        pairs = [(i, i ^ stride) for i in range(count)]
        blocks = blocks + [(k ^ stride, lax.ppermute(b, "tp", pairs)) for k, b in blocks]
        stride //= 2
    return blocks


def low_term(own, right, member, count):
    contract = (((0,), (0,)), ((), ()))
    if count & (count - 1):
        whole = lax.all_gather(own, "tp", axis=0, tiled=True)
        return lax.dot_general(whole, right, contract, preferred_element_type=jnp.float32)
    rows, total = own.shape[0], 0.0
    for k, block in token_blocks(own, count):
        cut = lax.dynamic_slice_in_dim(right, (member ^ k) * rows, rows, 0)
        total = total + lax.dot_general(
            block, cut, contract, preferred_element_type=jnp.float32
        )
    return total


def sum_over_mesh(value, counts):
    tile = jnp.full((8, 128), value)
    for axis, count in counts:
        if count & (count - 1):
            tile = lax.psum(tile, axis)
            continue
        stride = 1
        while stride < count:
            tile = tile + lax.ppermute(tile, axis, [(i, i ^ stride) for i in range(count)])
            stride *= 2
    return tile[0, 0]


def sum_scatter(terms, count):
    rows = terms.shape[1] // count
    me = lax.axis_index("fs")
    if count > UNROLL_LIMIT:
        return lax.psum_scatter(terms, "fs", scatter_dimension=1, tiled=True)
    total = lax.dynamic_slice_in_dim(terms, me * rows, rows, 1)
    sent = terms.astype(jnp.bfloat16)
    for shift in sorted(range(1, count), key=lambda k: -min(k, count - k)):
        piece = lax.dynamic_slice_in_dim(sent, ((me + shift) % count) * rows, rows, 1)
        pairs = [(i, (i + shift) % count) for i in range(count)]
        total = total + lax.ppermute(piece, "fs", pairs).astype(jnp.float32)
    return total


def on_device(
    block_input,
    gate_cotangent,
    gated_state,
    mixer_cotangent,
    gate_basis,
    out_basis,
    gate_master,
    out_master,
    gate_first,
    gate_second,
    out_first,
    out_second,
):
    low_rank = gate_basis.shape[1]
    local_cols = gate_first.shape[1]
    fs_count, tp_count = lax.axis_size("fs"), lax.axis_size("tp")
    member = lax.axis_index("tp")

    gate_old = lax.all_gather(gate_master.astype(jnp.bfloat16), "fs", axis=0, tiled=True)
    out_old = lax.all_gather(out_master.astype(jnp.bfloat16), "fs", axis=1, tiled=True)

    own_in, own_cot, gate_whole, out_whole = project(
        block_input, mixer_cotangent, gate_basis, out_basis, fs_count, tp_count
    )
    gate_term = low_term(own_in.astype(jnp.bfloat16), gate_cotangent, member, tp_count)
    out_term = low_term(own_cot.astype(jnp.bfloat16), gated_state, member, tp_count)
    low = sum_scatter(jnp.stack([gate_term, out_term]), fs_count)
    gate_low, out_low = low[0], low[1]

    gate_first_new = 0.9 * gate_first + 0.1 * gate_low
    out_first_new = 0.9 * out_first + 0.1 * out_low
    gate_second_new = 0.95 * gate_second + 0.05 * gate_low * gate_low
    out_second_new = 0.95 * out_second + 0.05 * out_low * out_low
    raw_gate = gate_first_new / jnp.sqrt(gate_second_new)
    raw_out = out_first_new / jnp.sqrt(out_second_new)

    own_squares = jnp.sum(raw_gate * raw_gate + raw_out * raw_out)
    full_step = gather_steps(jnp.stack([raw_gate, raw_out]).astype(jnp.bfloat16), fs_count)
    squares = sum_over_mesh(own_squares, (("tp", tp_count), ("fs", fs_count)))
    norm_scale = lax.rsqrt(squares / (2.0 * low_rank * local_cols * tp_count) + 1e-06)
    rate = 0.25 * norm_scale

    full_gate, full_out = full_step[0], full_step[1]
    across = (((0,), (1,)), ((), ()))
    gate_copy = gate_old.astype(jnp.float32) - rate * jnp.dot(
        gate_whole, full_gate, preferred_element_type=jnp.float32
    )
    out_copy = out_old.astype(jnp.float32) - rate * lax.dot_general(
        full_out, out_whole, across, preferred_element_type=jnp.float32
    )
    gate_master_new = gate_master - rate * jnp.dot(
        gate_basis, full_gate, preferred_element_type=jnp.float32
    )
    out_master_new = out_master - rate * lax.dot_general(
        full_out, out_basis, across, preferred_element_type=jnp.float32
    )
    return (
        gate_master_new,
        out_master_new,
        gate_copy.astype(jnp.bfloat16),
        out_copy.astype(jnp.bfloat16),
        gate_first_new,
        gate_second_new,
        out_first_new,
        out_second_new,
    )


def solution(mesh):
    return jax.shard_map(
        on_device,
        mesh=mesh,
        in_specs=(
            P(("fs", "tp"), None),
            P("fs", "tp"),
            P("fs", "tp"),
            P(("fs", "tp"), None),
            P("fs", None),
            P("fs", None),
            P("fs", "tp"),
            P("tp", "fs"),
            P("fs", "tp"),
            P("fs", "tp"),
            P("fs", "tp"),
            P("fs", "tp"),
        ),
        out_specs=(
            P("fs", "tp"),
            P("tp", "fs"),
            P(None, "tp"),
            P("tp", None),
            P("fs", "tp"),
            P("fs", "tp"),
            P("fs", "tp"),
            P("fs", "tp"),
        ),
        check_vma=False,
    )
```

```python
import jax
import jax.numpy as jnp
from jax import lax
from jax.sharding import PartitionSpec as P


UNROLL_LIMIT = 16


def ring_order(count):
    return list(range(0, count, 2)) + list(range(1, count, 2))[::-1]


def place_on(axis):
    return lax.axis_index(axis).astype(jnp.uint32)


def ring_chunks(own, axis, count, dim):
    order = ring_order(count)
    forward = [(order[p], order[(p + 1) % count]) for p in range(count)]
    backward = [(b, a) for a, b in forward]
    me = lax.axis_index(axis)
    steps = [-s if up else s for s in range(1, count // 2) for up in (True, False)]
    steps.append(count // 2)
    table = [[order[(order.index(i) + s) % count] for s in steps] for i in range(count)]
    owners = lax.dynamic_index_in_dim(jnp.asarray(table, jnp.uint32), me, 0, keepdims=False)
    size = own.shape[dim]
    half = size // 2
    up = down = own
    chunks = []
    for step in range(1, count // 2):
        up = lax.ppermute(up, axis, forward)
        down = lax.ppermute(down, axis, backward)
        chunks.append((owners[2 * step - 2], 0, up))
        chunks.append((owners[2 * step - 1], 0, down))
    first = lax.slice_in_dim(up, 0, half, axis=dim)
    last = lax.slice_in_dim(down, half, size, axis=dim)
    chunks.append((owners[count - 2], 0, lax.ppermute(first, axis, forward)))
    chunks.append((owners[count - 2], half, lax.ppermute(last, axis, backward)))
    return chunks


def gather_steps(own, count):
    if count % 2 or count > UNROLL_LIMIT:
        return lax.all_gather(own, "fs", axis=1, tiled=True)
    kinds, rows, cols = own.shape
    zero = jnp.uint32(0)
    whole = jnp.zeros((kinds, count * rows, cols), own.dtype)
    whole = lax.dynamic_update_slice(whole, own, (zero, place_on("fs") * rows, zero))
    for owner, start, chunk in ring_chunks(own, "fs", count, 1):
        whole = lax.dynamic_update_slice(whole, chunk, (zero, owner * rows + start, zero))
    return whole


def gather_bases(gate_basis, out_basis, fs_count, tp_count):
    if fs_count % 2 or tp_count % 2 or fs_count > UNROLL_LIMIT:
        return (
            lax.all_gather(gate_basis, "fs", axis=0, tiled=True),
            lax.all_gather(out_basis, "fs", axis=0, tiled=True),
        )
    rows, cols = gate_basis.shape
    parity, zero = place_on("tp") & 1, jnp.uint32(0)
    swap = [(i, i ^ 1) for i in range(tp_count)]
    own = jnp.where(parity == 0, gate_basis, out_basis)
    wholes = jnp.zeros((2, fs_count * rows, cols), gate_basis.dtype)
    at = place_on("fs") * rows
    pair = jnp.stack([gate_basis, out_basis])
    wholes = lax.dynamic_update_slice(wholes, pair, (zero, at, zero))
    for owner, start, chunk in ring_chunks(own, "fs", fs_count, 0):
        other = lax.ppermute(chunk, "tp", swap)
        at = owner * rows + start
        wholes = lax.dynamic_update_slice(wholes, chunk[None], (parity, at, zero))
        wholes = lax.dynamic_update_slice(wholes, other[None], (parity ^ 1, at, zero))
    return wholes[0], wholes[1]


def token_blocks(own, count):
    blocks, stride = [(0, own)], count // 2
    while stride:
        pairs = [(i, i ^ stride) for i in range(count)]
        blocks = blocks + [(k ^ stride, lax.ppermute(b, "tp", pairs)) for k, b in blocks]
        stride //= 2
    return blocks


def low_term(own, right, member, count):
    contract = (((0,), (0,)), ((), ()))
    if count & (count - 1):
        whole = lax.all_gather(own, "tp", axis=0, tiled=True)
        return lax.dot_general(whole, right, contract, preferred_element_type=jnp.float32)
    rows, total = own.shape[0], 0.0
    for k, block in token_blocks(own, count):
        cut = lax.dynamic_slice_in_dim(right, (member ^ k) * rows, rows, 0)
        total = total + lax.dot_general(
            block, cut, contract, preferred_element_type=jnp.float32
        )
    return total


def sum_scatter(terms, count):
    if count % 2 or count > UNROLL_LIMIT:
        return lax.psum_scatter(terms, "fs", scatter_dimension=0, tiled=True)
    cols, outer = terms.shape[1], count // 2
    rows = terms.shape[0] // count
    me = place_on("fs")
    side, place, zero = me & 1, me >> 1, jnp.uint32(0)
    terms = terms.reshape(outer, 2, rows, cols)
    shape = (outer, 1, rows, cols)
    kept = lax.dynamic_slice(terms, (zero, side, zero, zero), shape)[:, 0]
    sent = lax.dynamic_slice(terms, (zero, side ^ 1, zero, zero), shape)[:, 0]
    swap = [(i, i ^ 1) for i in range(count)]
    taken = lax.ppermute(sent.astype(jnp.bfloat16), "fs", swap)
    both = kept + taken.astype(jnp.float32)
    total = lax.dynamic_index_in_dim(both, place, 0, keepdims=False)
    sent = both.astype(jnp.bfloat16)
    for shift in sorted(range(1, outer), key=lambda k: -min(k, outer - k)):
        to = lax.rem(place + jnp.uint32(shift), jnp.uint32(outer))
        piece = lax.dynamic_index_in_dim(sent, to, 0, keepdims=False)
        pairs = [(i, (i + 2 * shift) % count) for i in range(count)]
        total = total + lax.ppermute(piece, "fs", pairs).astype(jnp.float32)
    return total


def on_device(
    block_input,
    gate_cotangent,
    gated_state,
    mixer_cotangent,
    gate_basis,
    out_basis,
    gate_master,
    out_master,
    gate_first,
    gate_second,
    out_first,
    out_second,
):
    low_rank = gate_basis.shape[1]
    local_cols = gate_first.shape[1]
    fs_count, tp_count = lax.axis_size("fs"), lax.axis_size("tp")
    member = place_on("tp")

    gate_old = lax.all_gather(gate_master.astype(jnp.bfloat16), "fs", axis=0, tiled=True)
    out_old = lax.all_gather(out_master.astype(jnp.bfloat16), "fs", axis=1, tiled=True)

    gate_whole, out_whole = gather_bases(gate_basis, out_basis, fs_count, tp_count)
    own_in = jnp.dot(block_input, gate_whole, preferred_element_type=jnp.float32)
    own_cot = jnp.dot(mixer_cotangent, out_whole, preferred_element_type=jnp.float32)
    gate_term = low_term(own_in.astype(jnp.bfloat16), gate_cotangent, member, tp_count)
    out_term = low_term(own_cot.astype(jnp.bfloat16), gated_state, member, tp_count)
    gate_low, out_low = sum_scatter(gate_term, fs_count), sum_scatter(out_term, fs_count)

    gate_first_new = 0.9 * gate_first + 0.1 * gate_low
    out_first_new = 0.9 * out_first + 0.1 * out_low
    gate_second_new = 0.95 * gate_second + 0.05 * gate_low * gate_low
    out_second_new = 0.95 * out_second + 0.05 * out_low * out_low
    raw_gate = gate_first_new / jnp.sqrt(gate_second_new)
    raw_out = out_first_new / jnp.sqrt(out_second_new)

    raw_step = jnp.stack([raw_gate, raw_out]).astype(jnp.bfloat16)
    full_step = gather_steps(raw_step, fs_count)
    wide_step = full_step.astype(jnp.float32)
    squares = jnp.full((8, 128), jnp.sum(wide_step * wide_step))
    parts = [squares]
    for shift in range(1, tp_count):
        pairs = [(i, (i + shift) % tp_count) for i in range(tp_count)]
        parts.append(lax.ppermute(squares, "tp", pairs))
    squares = sum(parts)[0, 0]
    norm_scale = lax.rsqrt(squares / (2.0 * low_rank * local_cols * tp_count) + 1e-06)
    rate = 0.25 * norm_scale

    full_gate, full_out = full_step[0], full_step[1]
    across = (((0,), (1,)), ((), ()))
    gate_copy = gate_old.astype(jnp.float32) - rate * jnp.dot(
        gate_whole, full_gate, preferred_element_type=jnp.float32
    )
    out_copy = out_old.astype(jnp.float32) - rate * lax.dot_general(
        full_out, out_whole, across, preferred_element_type=jnp.float32
    )
    gate_master_new = gate_master - rate * jnp.dot(
        gate_basis, full_gate, preferred_element_type=jnp.float32
    )
    out_master_new = out_master - rate * lax.dot_general(
        full_out, out_basis, across, preferred_element_type=jnp.float32
    )
    return (
        gate_master_new,
        out_master_new,
        gate_copy.astype(jnp.bfloat16),
        out_copy.astype(jnp.bfloat16),
        gate_first_new,
        gate_second_new,
        out_first_new,
        out_second_new,
    )


def solution(mesh):
    return jax.shard_map(
        on_device,
        mesh=mesh,
        in_specs=(
            P(("fs", "tp"), None),
            P("fs", "tp"),
            P("fs", "tp"),
            P(("fs", "tp"), None),
            P("fs", None),
            P("fs", None),
            P("fs", "tp"),
            P("tp", "fs"),
            P("fs", "tp"),
            P("fs", "tp"),
            P("fs", "tp"),
            P("fs", "tp"),
        ),
        out_specs=(
            P("fs", "tp"),
            P("tp", "fs"),
            P(None, "tp"),
            P("tp", None),
            P("fs", "tp"),
            P("fs", "tp"),
            P("fs", "tp"),
            P("fs", "tp"),
        ),
        check_vma=False,
    )
```
